32 devices in a mesh: sp: 8 (over z, core), tp: 4 (over y, x).
Axes of the slice: x: 2, y: 2, z: 4, core: 2. Of those that a mesh axis runs over, the one named last changes fastest.
Arguments:
- residual: bfloat16 [896, 2048], P('sp'), may hold values from -1.5 to 1.5
- latent: bfloat16 [896, 512], P('sp'), may hold values from -6 to 6
- rot_key: bfloat16 [896, 64], P('sp'), may hold values from -6 to 6
- latent_norm_scale: float32 [512], replicated, may hold values from 0.1 to 1.9
- query_wide: bfloat16 [896, 3072], P('sp', 'tp'), may hold values from -210 to 210
- query_narrow: bfloat16 [896, 2048], P('sp', 'tp'), may hold values from -210 to 210
- large_key_lift: bfloat16 [512, 2048], P(None, 'tp'), may hold values from -0.25 to 0.25
- large_value_lift: bfloat16 [512, 2048], P(None, 'tp'), may hold values from -0.25 to 0.25
- small_key_lift: bfloat16 [512, 1024], P(None, 'tp'), may hold values from -0.25 to 0.25
- small_value_lift: bfloat16 [512, 1024], P(None, 'tp'), may hold values from -0.25 to 0.25
- out_wide: bfloat16 [2048, 2048], P('tp'), may hold values from -0.5 to 0.5
- out_narrow: bfloat16 [1024, 2048], P('tp'), may hold values from -0.75 to 0.75
- mix_gain: float32 [2048], replicated, may hold values from 0.1 to 1.9
- router_group: bfloat16 [2048, 4], replicated, may hold values from -0.125 to 0.125
- router_expert: bfloat16 [2048, 8], replicated, may hold values from -0.125 to 0.125
- expert_ids: int32 [896, 2], P('sp'), may hold values from 0 to 7, all different within a row; in each aligned block of 112 rows (0 to 111, 112 to 223, ...) at most 56 rows name the same one
- expert_gate_w: bfloat16 [8, 2048, 4096], P('sp', None, 'tp'), may hold values from -0.125 to 0.125
- expert_up_w: bfloat16 [8, 2048, 4096], P('sp', None, 'tp'), may hold values from -0.125 to 0.125
- expert_down_w: bfloat16 [8, 4096, 2048], P('sp', 'tp'), may hold values from -0.375 to 0.375
Outputs:
- updated: bfloat16 [896, 2048], P('sp', 'tp')
The draws below stay inside these ranges and needn't reach their ends.
Inputs may be any that keep to these rules, and one draw needn't show every extreme that they name: `expert_ids`: each row names two different experts; the rows of one index of sp name no expert more than 56 times, a bound that some expert reaches in some of these blocks.
All inputs are finite; a program needn't handle non-finite values.
Results may differ from the reference program's by a relative error of at most 0.024.
The reference program's roundings to bfloat16 on the way count: a program that leaves them out, or rounds other values in their place, can miss the bound.
Values may be sent and summed in bfloat16 or wider, within the bound.
A program may use at most 64 MiB of HBM per device.

```python
import math
import jax
import jax.numpy as jnp
import numpy as np
from jax import lax

D = 2048
LARGE_HEADS = 16
SMALL_HEADS = 16
PLAIN_KEY_WIDTH = 128
LARGE_VALUE_SIZE = 128
SMALL_HEAD_WIDTH = 64
ROPE = 64
LATENT_WIDTH = 512
GROUPS = 4
FF = 4096
TOK_DEV = 112
EXPERTS = 8
EXP_GROUP = 2
TOKEN_TOTAL = 896
CAP = 56
N_SP = 8
N_TP = 4


def spiked_queries(key, head_count, plain_width):
    columns = head_count * (plain_width + ROPE)
    base_key = jax.random.fold_in(jax.random.fold_in(key, 11), 0)
    values = jnp.clip(jax.random.normal(base_key, (TOKEN_TOTAL, columns), jnp.float32), -4.0, 4.0)
    return values.astype(jnp.bfloat16)


def draw_query_wide(key, part):
    return spiked_queries(jax.random.fold_in(key, 3), LARGE_HEADS, PLAIN_KEY_WIDTH)


def draw_query_narrow(key, part):
    return spiked_queries(jax.random.fold_in(key, 5), SMALL_HEADS, SMALL_HEAD_WIDTH)


def level_of(rng, extent, pieces, low, top_value):
    loudness, own = 1.0, jax.random.fold_in(rng, 6)
    for position, blocks in pieces:
        draws = jnp.exp(jax.random.uniform(jax.random.fold_in(own, position), (blocks,), jnp.float32, low / len(pieces), top_value / len(pieces)))
        loudness = loudness * jnp.repeat(draws, extent[position] // blocks).reshape([-1 if axis == position else 1 for axis in range(len(extent))])
    return loudness


def deal_out(rng, own, number, rows, amount, top, most, skew):
    sequence = jax.random.permutation(rng, amount)
    packed, ordinary = portions_of(amount, rows * top, most, skew, True), portions_of(amount, rows * top, most, skew, False)
    places = jnp.arange(amount)

    def named(tallies, rotation):
        used = int((tallies > 0).sum())
        fixed = max(1, used // 4)
        moved = fixed + (places - fixed + rotation * (used - fixed)) % max(1, amount - fixed)
        return jnp.zeros((amount,), jnp.int32).at[sequence[jnp.where(places < fixed, places, moved)]].set(jnp.asarray(tallies, jnp.int32))

    tallies = jnp.where(number % 4 == 0, named(packed, number // 4), named(ordinary, number - number // 4 - 1))
    mixed = jax.random.permutation(jax.random.fold_in(own, 3), amount)
    donor, sink = mixed[0:amount // 2 * 2:2], mixed[1:amount // 2 * 2:2]
    margin = jnp.minimum(tallies[donor] - 1, most - tallies[sink]) // 2
    margin = jnp.where((donor == sequence[0]) | (sink == sequence[0]) | (tallies[sink] == 0), 0, jnp.maximum(margin, 0))
    moved = jax.random.randint(jax.random.fold_in(own, 4), (amount // 2,), 0, 1 << 20) % (margin + 1)
    tallies = tallies.at[donor].add(-moved).at[sink].add(moved)
    members = jnp.searchsorted(jnp.cumsum(tallies), jnp.arange(rows * top), side="right").astype(jnp.int32)
    grid = members.reshape(top, rows).T
    grid = grid[jax.random.permutation(jax.random.fold_in(own, 1), rows)]
    rotation = jax.random.randint(jax.random.fold_in(own, 2), (rows, 1), 0, top)
    return jnp.take_along_axis(grid, (jnp.arange(top)[None, :] + rotation) % top, axis=1)


def portions_of(amount, total, bound, lean, full):
    portions = [(1 << 20) // math.isqrt(grade ** lean) + 1 for grade in range(1, amount + 1)]
    largest = bound if full else min(bound, max(-(-total // amount), total * portions[0] // sum(portions)))
    least = 1 if total - largest >= amount - 1 else 0
    given, rest = [largest] + [least] * (amount - 1), total - largest - least * (amount - 1)
    while rest > 0:
        candidates = [i for i in range(1, amount) if given[i] < largest] or [i for i in range(1, amount) if given[i] < bound]
        whole, budget = sum([portions[i] for i in candidates]), rest
        for i in candidates:
            more = min(bound - given[i], max(1, budget * portions[i] // whole), rest)
            given[i] = given[i] + more
            rest = rest - more
    return np.array(given)


def centred(key, extent, deviation, limit, cuts=(), held_as=jnp.bfloat16):
    array = deviation * jax.random.normal(key, extent, jnp.float32)
    if cuts:
        array = array * level_of(key, extent, cuts, -0.22, 0.18)
    return jnp.clip(array, -limit, limit).astype(held_as)


def setup_inputs(seed: int = 0) -> dict:
    splits = jax.random.split(jax.random.key(seed), 20)
    residual = centred(splits[0], (TOKEN_TOTAL, D), 0.25, 1.5, ((0, 8),))
    latent = centred(splits[1], (TOKEN_TOTAL, LATENT_WIDTH), 1.0, 6.0, ((0, 8),))
    rot_key = centred(splits[2], (TOKEN_TOTAL, ROPE), 1.0, 6.0, ((0, 8),))
    latent_norm_scale = jnp.clip(1.0 + 0.18 * jax.random.normal(splits[3], (LATENT_WIDTH,), jnp.float32), 0.1, 1.9)
    query_wide = draw_query_wide(jax.random.fold_in(splits[19], 71), 0)
    query_narrow = draw_query_narrow(jax.random.fold_in(splits[19], 71), 0)
    large_key_lift = centred(splits[6], (LATENT_WIDTH, LARGE_HEADS * PLAIN_KEY_WIDTH), LATENT_WIDTH ** -0.5, 0.25, ((1, 4),))
    large_value_lift = centred(splits[7], (LATENT_WIDTH, LARGE_HEADS * LARGE_VALUE_SIZE), LATENT_WIDTH ** -0.5, 0.25, ((1, 4),))
    small_key_lift = centred(splits[8], (LATENT_WIDTH, SMALL_HEADS * SMALL_HEAD_WIDTH), LATENT_WIDTH ** -0.5, 0.25, ((1, 4),))
    small_value_lift = centred(splits[9], (LATENT_WIDTH, SMALL_HEADS * SMALL_HEAD_WIDTH), LATENT_WIDTH ** -0.5, 0.25, ((1, 4),))
    out_wide = centred(splits[10], (LARGE_HEADS * LARGE_VALUE_SIZE, D), LARGE_VALUE_SIZE ** -0.5, 0.5, ((0, 4),))
    out_narrow = centred(splits[11], (SMALL_HEADS * SMALL_HEAD_WIDTH, D), SMALL_HEAD_WIDTH ** -0.5, 0.75, ((0, 4),))
    mix_gain = jnp.clip(1.0 + 0.18 * jax.random.normal(splits[12], (D,), jnp.float32), 0.1, 1.9)
    router_group = centred(splits[13], (D, GROUPS), D ** -0.5, 0.125)
    router_expert = centred(splits[14], (D, EXPERTS), D ** -0.5, 0.125)
    expert_ids_keys = jax.random.split(jax.random.fold_in(splits[15], 1), TOKEN_TOTAL // TOK_DEV)
    expert_ids_turns = jax.random.permutation(jax.random.fold_in(splits[15], 3), TOKEN_TOTAL // TOK_DEV)
    expert_ids = jax.vmap(lambda own, number: deal_out(jax.random.fold_in(splits[15], 2), own, number, TOK_DEV, EXPERTS, 2, CAP, 1))(expert_ids_keys, expert_ids_turns).reshape((TOKEN_TOTAL, 2))
    expert_gate_w = centred(splits[16], (EXPERTS, D, FF), D ** -0.5, 0.125, ((0, 8), (2, 4)))
    expert_up_w = centred(splits[17], (EXPERTS, D, FF), D ** -0.5, 0.125, ((0, 8), (2, 4)))
    expert_down_w = centred(splits[18], (EXPERTS, FF, D), (FF // 16) ** -0.5, 0.375, ((0, 8), (1, 4)))
    return dict(residual=residual, latent=latent, rot_key=rot_key, latent_norm_scale=latent_norm_scale, query_wide=query_wide, query_narrow=query_narrow, large_key_lift=large_key_lift, large_value_lift=large_value_lift, small_key_lift=small_key_lift, small_value_lift=small_value_lift, out_wide=out_wide, out_narrow=out_narrow, mix_gain=mix_gain, router_group=router_group, router_expert=router_expert, expert_ids=expert_ids, expert_gate_w=expert_gate_w, expert_up_w=expert_up_w, expert_down_w=expert_down_w)


rope_base = 10000.0
epsilon = 1e-06
very_low = -1e+30

def angle_table(positions, width):
    frequency = rope_base ** (-jnp.arange(0, width, 2, dtype=jnp.float32) / width)
    return positions.astype(jnp.float32)[:, None] * frequency[None, :]

def rotate(values, angles):
    half_width = values.shape[-1] // 2
    cosine = jnp.cos(angles)
    sine_part = jnp.sin(angles)
    front_half = values[..., :half_width]
    back_half = values[..., half_width:]
    return jnp.concatenate([front_half * cosine - back_half * sine_part, front_half * sine_part + back_half * cosine], axis=-1)

def rms_scale(values, gain):
    return values * lax.rsqrt(lax.optimization_barrier(jnp.mean(values * values, axis=-1, keepdims=True)) + epsilon) * gain

def roped_queries(query, plain_width, angles):
    row_count = query.shape[0]
    shaped = query.reshape(row_count, -1, plain_width + ROPE)
    turned = rotate(shaped[..., plain_width:].astype(jnp.float32), angles[:, None, :]).astype(jnp.bfloat16)
    return jnp.concatenate([shaped[..., :plain_width], turned], axis=-1)

def expand_keys(latent_rows, large_key_lift, large_value_lift, small_key_lift, small_value_lift):
    row_count = latent_rows.shape[0]

    def project(weight, head_width):
        product = jnp.dot(latent_rows, weight, preferred_element_type=jnp.float32).astype(jnp.bfloat16)
        return product.reshape(row_count, weight.shape[1] // head_width, head_width)
    return (project(large_key_lift, PLAIN_KEY_WIDTH), project(large_value_lift, LARGE_VALUE_SIZE), project(small_key_lift, SMALL_HEAD_WIDTH), project(small_value_lift, SMALL_HEAD_WIDTH))

def attention_group(queries, key_rows, value_rows, key_rot, plain_width):
    token_count = queries.shape[0]
    score_scale = (plain_width + ROPE) ** (-0.5)
    causal_mask = jnp.arange(token_count)[:, None] >= jnp.arange(token_count)[None, :]

    def one_head(inputs):
        query_head, key_head, value_head = inputs
        scores = jnp.dot(query_head[:, :plain_width], key_head.T, preferred_element_type=jnp.float32)
        scores = scores + jnp.dot(query_head[:, plain_width:], key_rot.T, preferred_element_type=jnp.float32)
        scores = scores * score_scale
        row_peak = lax.optimization_barrier(jnp.max(jnp.where(causal_mask, scores, very_low), axis=1, keepdims=True))
        weights = jnp.where(causal_mask, jnp.exp(scores - row_peak), 0.0)
        weight_sum = lax.optimization_barrier(jnp.sum(weights, axis=1, keepdims=True))
        mixed_values = jnp.dot(weights.astype(jnp.bfloat16), value_head, preferred_element_type=jnp.float32)
        return (mixed_values / weight_sum).astype(jnp.bfloat16)
    result = lax.map(one_head, (queries.transpose(1, 0, 2), key_rows.transpose(1, 0, 2), value_rows.transpose(1, 0, 2)))
    return result.transpose(1, 0, 2).reshape(token_count, -1)

def reference(residual, latent, rot_key, latent_norm_scale, query_wide, query_narrow, large_key_lift, large_value_lift, small_key_lift, small_value_lift, out_wide, out_narrow, mix_gain, router_group, router_expert, expert_ids, expert_gate_w, expert_up_w, expert_down_w):
    token_count = latent.shape[0]
    positions = jnp.arange(token_count, dtype=jnp.int32)
    angles = angle_table(positions, ROPE)
    normed = rms_scale(latent.astype(jnp.float32), latent_norm_scale).astype(jnp.bfloat16)
    key_turned = rotate(rot_key.astype(jnp.float32), angles).astype(jnp.bfloat16)
    wide_queries = roped_queries(query_wide, PLAIN_KEY_WIDTH, angles)
    narrow_queries = roped_queries(query_narrow, SMALL_HEAD_WIDTH, angles)
    key_set = expand_keys(normed, large_key_lift, large_value_lift, small_key_lift, small_value_lift)
    heads_wide = attention_group(wide_queries, key_set[0], key_set[1], key_turned, PLAIN_KEY_WIDTH)
    heads_narrow = attention_group(narrow_queries, key_set[2], key_set[3], key_turned, SMALL_HEAD_WIDTH)

    def head_blocks(values):
        return values.reshape(token_count, N_TP, -1).transpose(1, 0, 2)

    def add_block(running, inputs):
        wide_block, wide_weight, narrow_block, narrow_weight = inputs
        partial_value = jnp.dot(wide_block, wide_weight, preferred_element_type=jnp.float32)
        partial_value = partial_value + jnp.dot(narrow_block, narrow_weight, preferred_element_type=jnp.float32)
        rounded = lax.optimization_barrier(partial_value.astype(jnp.bfloat16)).astype(jnp.float32)
        return (running + rounded, None)
    attended, ignored = lax.scan(add_block, jnp.zeros((token_count, D), jnp.float32), (head_blocks(heads_wide), out_wide.reshape(N_TP, -1, D), head_blocks(heads_narrow), out_narrow.reshape(N_TP, -1, D)))
    mixed = residual.astype(jnp.float32) + attended
    normal_rows = rms_scale(mixed, mix_gain).astype(jnp.bfloat16)
    group_prob = jax.nn.softmax(jnp.dot(normal_rows, router_group, preferred_element_type=jnp.float32), axis=-1)
    logits = jnp.dot(normal_rows, router_expert, preferred_element_type=jnp.float32)
    chosen_group = expert_ids[:, 0] // EXP_GROUP
    group_pick = lax.optimization_barrier(jnp.sum(jnp.where(chosen_group[:, None] == jnp.arange(GROUPS)[None, :], group_prob, 0.0), axis=1))
    expert_match = expert_ids[:, :, None] == jnp.arange(EXPERTS)[None, None, :]
    chosen_logits = lax.optimization_barrier(jnp.sum(jnp.where(expert_match, logits[:, None, :], 0.0), axis=2))
    gates = group_pick[:, None] * jax.nn.softmax(chosen_logits, axis=-1)
    block_ids = expert_ids.reshape(N_SP, -1)
    one_hot = (block_ids[:, :, None] == jnp.arange(EXPERTS)[None, None, :]).astype(jnp.int32)
    earlier = jnp.cumsum(one_hot, axis=1) - one_hot
    slot_index = lax.optimization_barrier(jnp.sum(earlier * one_hot, axis=2))
    block_index = jnp.arange(N_SP, dtype=jnp.int32)[:, None]
    target = (block_ids * (N_SP * CAP) + block_index * CAP + slot_index).reshape(-1).astype(jnp.int32)
    source_row = jnp.arange(2 * token_count, dtype=jnp.int32) // 2
    slot_total = EXPERTS * N_SP * CAP
    row_of_slot = jnp.zeros((slot_total,), jnp.int32).at[target].set(source_row)
    slot_used = jnp.zeros((slot_total,), jnp.bool_).at[target].set(True)

    def run_expert(inputs):
        rows_index, used, gate_weight, up_weight, down_weight = inputs
        expert_rows = jnp.where(used[:, None], normal_rows[rows_index], jnp.zeros((), jnp.bfloat16))
        gate_part = jnp.dot(expert_rows, gate_weight, preferred_element_type=jnp.float32)
        up_part = jnp.dot(expert_rows, up_weight, preferred_element_type=jnp.float32)
        hidden = (jax.nn.silu(gate_part) * up_part).astype(jnp.bfloat16)
        hidden_blocks = hidden.astype(jnp.float32).reshape(hidden.shape[0], N_TP, -1)
        down_blocks = down_weight.astype(jnp.float32).reshape(N_TP, -1, D)
        partials = jnp.einsum('rjf,jfd->jrd', hidden_blocks, down_blocks)
        rounded = lax.optimization_barrier(partials.astype(jnp.bfloat16)).astype(jnp.float32)
        return lax.optimization_barrier(jnp.sum(rounded, axis=0)).astype(jnp.bfloat16)
    expert_out = lax.map(run_expert, (row_of_slot.reshape(EXPERTS, -1), slot_used.reshape(EXPERTS, -1), expert_gate_w, expert_up_w, expert_down_w))
    picked = expert_out.reshape(slot_total, D)[target].astype(jnp.float32).reshape(token_count, 2, D)
    combined = lax.optimization_barrier(jnp.sum(picked * gates[:, :, None], axis=1))
    return (mixed + combined).astype(jnp.bfloat16)
```

```python
import functools

import jax
import jax.numpy as jnp
from jax import lax
from jax.experimental import pallas as pl
from jax.experimental.pallas import tpu as pltpu
from jax.sharding import PartitionSpec as P

PLAIN_KEY_WIDTH = 128
LARGE_VALUE_SIZE = 128
SMALL_HEAD_WIDTH = 64
ROPE = 64


rope_base = 10000.0
epsilon = 1e-06
very_low = -1e30


def angle_table(positions, width):
    frequency = rope_base ** (-jnp.arange(0, width, 2, dtype=jnp.float32) / width)
    return positions.astype(jnp.float32)[:, None] * frequency[None, :]


def rotate(values, angles):
    half_width = values.shape[-1] // 2
    cosine = jnp.cos(angles)
    sine_part = jnp.sin(angles)
    front_half = values[..., :half_width]
    back_half = values[..., half_width:]
    return jnp.concatenate(
        [front_half * cosine - back_half * sine_part, front_half * sine_part + back_half * cosine],
        axis=-1,
    )


def rms_scale(values, gain):
    return values * lax.rsqrt(jnp.mean(values * values, axis=-1, keepdims=True) + epsilon) * gain


def roped_queries(query, plain_width, angles):
    row_count = query.shape[0]
    shaped = query.reshape(row_count, -1, plain_width + ROPE)
    turned = rotate(shaped[..., plain_width:].astype(jnp.float32), angles[:, None, :]).astype(
        jnp.bfloat16
    )
    return jnp.concatenate([shaped[..., :plain_width], turned], axis=-1)


def expand_keys(latent_rows, large_key_lift, large_value_lift, small_key_lift, small_value_lift):
    row_count = latent_rows.shape[0]

    def project(weight, head_width):
        product = jnp.dot(latent_rows, weight, preferred_element_type=jnp.float32).astype(
            jnp.bfloat16
        )
        return product.reshape(row_count, weight.shape[1] // head_width, head_width)

    return (
        project(large_key_lift, PLAIN_KEY_WIDTH),
        project(large_value_lift, LARGE_VALUE_SIZE),
        project(small_key_lift, SMALL_HEAD_WIDTH),
        project(small_value_lift, SMALL_HEAD_WIDTH),
    )


def attend_group(state, queries, plain_width, key_rows, values, key_rot, causal_mask):
    row_peak, weight_sum, summed = state
    score_scale = (plain_width + ROPE) ** (-0.5)
    scores = jnp.einsum(
        "qhd,khd->qhk", queries[..., :plain_width], key_rows, preferred_element_type=jnp.float32
    )
    scores = scores + jnp.einsum(
        "qhd,kd->qhk", queries[..., plain_width:], key_rot, preferred_element_type=jnp.float32
    )
    scores = scores * score_scale
    allowed = causal_mask[:, None, :]
    new_peak = jnp.maximum(row_peak, jnp.max(jnp.where(allowed, scores, very_low), axis=-1))
    weights = jnp.where(allowed, jnp.exp(scores - new_peak[..., None]), 0.0)
    weight_sum = jnp.sum(weights, axis=-1)
    summed = jnp.einsum(
        "qhk,khd->qhd", weights.astype(jnp.bfloat16), values, preferred_element_type=jnp.float32
    )
    return (new_peak, weight_sum, summed)


MESH = pl.DeviceIdType.MESH
VMEM_SPEC = pl.BlockSpec(memory_space=pltpu.VMEM)


def flipped(index, bits):
    result, bit = index, 1
    while bit <= bits:
        if bits & bit:
            result = result + bit - 2 * bit * ((index // bit) % 2)
        bit *= 2
    return result


def peer_of(index, step, count):
    if count & (count - 1) == 0:
        return flipped(index, step)
    return lax.rem(index + step, count)


def source_of(index, step, count):
    if count & (count - 1) == 0:
        return flipped(index, step)
    return lax.rem(index + count - step, count)


def to(sp, tp):
    return {"sp": sp, "tp": tp}


def greet(partners):
    barrier = pltpu.get_barrier_semaphore()
    for partner in partners:
        pl.semaphore_signal(barrier, inc=1, device_id=partner, device_id_type=MESH)
    pl.semaphore_wait(barrier, len(partners))


def send(src, dst, send_sem, recv_sem, device):
    copy = pltpu.make_async_remote_copy(
        src_ref=src,
        dst_ref=dst,
        send_sem=send_sem,
        recv_sem=recv_sem,
        device_id=device,
        device_id_type=MESH,
    )
    copy.start()
    return copy


def arrival(dst, send_sem, recv_sem, device):
    pltpu.make_async_remote_copy(
        src_ref=dst,
        dst_ref=dst,
        send_sem=send_sem,
        recv_sem=recv_sem,
        device_id=device,
        device_id_type=MESH,
    ).wait_recv()


def gather_kernel(sp_count, x_ref, out_ref, send_sem, recv_sem):
    me, column = lax.axis_index("sp"), lax.axis_index("tp")
    chips = sp_count // 2
    chip, core = me // 2, me % 2
    partner = 2 * chip + 1 - core
    greet(
        [to(partner, column)]
        + [to(2 * peer_of(chip, d, chips) + core, column) for d in range(1, chips)]
    )
    copies = []
    for d in range(chips - 1, 0, -1):
        there = 2 * peer_of(chip, d, chips) + core
        copies.append(
            send(x_ref, out_ref.at[me], send_sem.at[d], recv_sem.at[me], to(there, column))
        )
    copies.append(
        send(x_ref, out_ref.at[me], send_sem.at[0], recv_sem.at[me], to(partner, column))
    )
    out_ref[me] = x_ref[...]
    for d in range(1, chips):
        origin = 2 * source_of(chip, d, chips) + core
        block = out_ref.at[origin]
        arrival(block, send_sem.at[chips + d], recv_sem.at[origin], to(partner, column))
        copies.append(
            send(block, block, send_sem.at[chips + d], recv_sem.at[origin], to(partner, column))
        )
    for d in range(chips):
        origin = 2 * source_of(chip, d, chips) + 1 - core
        arrival(
            out_ref.at[origin], send_sem.at[0], recv_sem.at[origin], to(partner, column)
        )
    for copy in copies:
        copy.wait_send()


def mix_kernel(
    tp_count,
    part_ref,
    residual_ref,
    gain_ref,
    router_ref,
    mixed_ref,
    stats_ref,
    held,
    own_stats,
    held_stats,
    send_sem,
    recv_sem,
):
    row, me = lax.axis_index("sp"), lax.axis_index("tp")
    width = mixed_ref.shape[1]
    greet([to(row, peer_of(me, d, tp_count)) for d in range(1, tp_count)])

    def columns(index):
        return pl.ds(pl.multiple_of(index * width, width), width)

    copies = []
    for d in range(1, tp_count):
        there = peer_of(me, d, tp_count)
        copies.append(
            send(
                part_ref.at[:, columns(there)],
                held.at[d],
                send_sem.at[0, d],
                recv_sem.at[0, d],
                to(row, there),
            )
        )
    total = residual_ref[:, columns(me)].astype(jnp.float32)
    total = total + part_ref[:, columns(me)].astype(jnp.float32)
    for d in range(1, tp_count):
        arrival(
            held.at[d],
            send_sem.at[0, d],
            recv_sem.at[0, d],
            to(row, peer_of(me, d, tp_count)),
        )
        total = total + held[d].astype(jnp.float32)
    mixed_ref[...] = total
    gained = (total * gain_ref[:, columns(me)]).astype(jnp.bfloat16)
    contract = (((1,), (1,)), ((), ()))
    router_rows = router_ref.shape[0]
    own_stats[:router_rows, :] = lax.dot_general(
        router_ref[:, columns(me)], gained, contract, preferred_element_type=jnp.float32
    )
    own_stats[router_rows:, :] = lax.dot_general(
        jnp.ones((8, width), jnp.float32),
        total * total,
        contract,
        precision=lax.Precision.HIGHEST,
        preferred_element_type=jnp.float32,
    )
    for d in range(1, tp_count):
        copies.append(
            send(
                own_stats,
                held_stats.at[d],
                send_sem.at[1, d],
                recv_sem.at[1, d],
                to(row, peer_of(me, d, tp_count)),
            )
        )
    stats = own_stats[...]
    for d in range(1, tp_count):
        arrival(
            held_stats.at[d],
            send_sem.at[1, d],
            recv_sem.at[1, d],
            to(row, peer_of(me, d, tp_count)),
        )
        stats = stats + held_stats[d]
    stats_ref[...] = stats
    for copy in copies:
        copy.wait_send()


def everyone(row, column, sp_count, tp_count):
    return [to(peer_of(row, d, sp_count), column) for d in range(1, sp_count)] + [
        to(row, peer_of(column, e, tp_count)) for e in range(1, tp_count)
    ]


def dispatch_kernel(
    sp_count, tp_count, x_ref, out_ref, line_send, line_recv, plane_send, plane_recv
):
    row, column = lax.axis_index("sp"), lax.axis_index("tp")
    width = x_ref.shape[2]
    greet(everyone(row, column, sp_count, tp_count))

    def place(origin, part):
        return out_ref.at[origin, :, pl.ds(pl.multiple_of(part * width, width), width)]

    copies = []
    for d in range(sp_count - 1, 0, -1):
        there = peer_of(row, d, sp_count)
        copies.append(
            send(
                x_ref.at[there],
                place(row, column),
                line_send.at[d],
                line_recv.at[d],
                to(there, column),
            )
        )
    for d in range(sp_count):
        origin = source_of(row, d, sp_count)
        block = place(origin, column)
        if d > 0:
            arrival(block, line_send.at[d], line_recv.at[d], to(origin, column))
        source = block if d > 0 else x_ref.at[row]
        for e in range(1, tp_count):
            copies.append(
                send(
                    source,
                    block,
                    plane_send.at[d, e],
                    plane_recv.at[d, e],
                    to(row, peer_of(column, e, tp_count)),
                )
            )
        if d == 0:
            out_ref[row, :, pl.ds(pl.multiple_of(column * width, width), width)] = x_ref[row]
    for d in range(sp_count):
        origin = source_of(row, d, sp_count)
        for e in range(1, tp_count):
            part = source_of(column, e, tp_count)
            arrival(
                place(origin, part),
                plane_send.at[d, e],
                plane_recv.at[d, e],
                to(row, part),
            )
    for copy in copies:
        copy.wait_send()


def combine_kernel(
    sp_count,
    tp_count,
    x_ref,
    out_ref,
    held,
    summed,
    line_send,
    line_recv,
    plane_send,
    plane_recv,
):
    row, column = lax.axis_index("sp"), lax.axis_index("tp")
    width = out_ref.shape[2]
    greet(everyone(row, column, sp_count, tp_count))

    def columns(part):
        return pl.ds(pl.multiple_of(part * width, width), width)

    copies = []
    for d in range(sp_count - 1, -1, -1):
        owner = peer_of(row, d, sp_count)
        for e in range(1, tp_count):
            there = peer_of(column, e, tp_count)
            copies.append(
                send(
                    x_ref.at[owner, :, columns(there)],
                    held.at[d, e],
                    plane_send.at[d, e],
                    plane_recv.at[d, e],
                    to(row, there),
                )
            )
    for d in range(sp_count - 1, -1, -1):
        owner = peer_of(row, d, sp_count)
        total = x_ref[owner, :, columns(column)].astype(jnp.float32)
        for e in range(1, tp_count):
            arrival(
                held.at[d, e],
                plane_send.at[d, e],
                plane_recv.at[d, e],
                to(row, source_of(column, e, tp_count)),
            )
            total = total + held[d, e].astype(jnp.float32)
        if d == 0:
            out_ref[row] = total.astype(jnp.bfloat16)
        else:
            summed[d] = total.astype(jnp.bfloat16)
            copies.append(
                send(
                    summed.at[d],
                    out_ref.at[row],
                    line_send.at[d],
                    line_recv.at[d],
                    to(owner, column),
                )
            )
    for d in range(1, sp_count):
        origin = source_of(row, d, sp_count)
        arrival(out_ref.at[origin], line_send.at[d], line_recv.at[d], to(origin, column))
    for copy in copies:
        copy.wait_send()


def call(body, out_shape, scratch, collective_id, *operands):
    many = isinstance(out_shape, (list, tuple))
    return pl.pallas_call(
        body,
        out_shape=out_shape,
        in_specs=[VMEM_SPEC] * len(operands),
        out_specs=[VMEM_SPEC] * len(out_shape) if many else VMEM_SPEC,
        scratch_shapes=scratch,
        compiler_params=pltpu.CompilerParams(
            collective_id=collective_id, has_side_effects=True
        ),
    )(*operands)


def shards(
    residual,
    latent,
    rot_key,
    latent_norm_scale,
    query_wide,
    query_narrow,
    large_key_lift,
    large_value_lift,
    small_key_lift,
    small_value_lift,
    out_wide,
    out_narrow,
    mix_gain,
    router_group,
    router_expert,
    expert_ids,
    expert_gate_w,
    expert_up_w,
    expert_down_w,
):
    tok_rows = latent.shape[0]
    positions = lax.axis_index("sp") * tok_rows + jnp.arange(tok_rows, dtype=jnp.int32)
    angles = angle_table(positions, ROPE)
    normed = rms_scale(latent.astype(jnp.float32), latent_norm_scale).astype(jnp.bfloat16)
    key_turned = rotate(rot_key.astype(jnp.float32), angles).astype(jnp.bfloat16)
    wide_queries = roped_queries(query_wide, PLAIN_KEY_WIDTH, angles)
    narrow_queries = roped_queries(query_narrow, SMALL_HEAD_WIDTH, angles)

    def empty_state(head_count, head_width):
        return (
            jnp.full((tok_rows, head_count), very_low, jnp.float32),
            jnp.zeros((tok_rows, head_count), jnp.float32),
            jnp.zeros((tok_rows, head_count, head_width), jnp.float32),
        )

    initial = (
        empty_state(wide_queries.shape[1], LARGE_VALUE_SIZE),
        empty_state(narrow_queries.shape[1], SMALL_HEAD_WIDTH),
    )
    sp_size, tp_size = lax.axis_size("sp"), lax.axis_size("tp")
    latent_width = latent.shape[1]
    dma = pltpu.SemaphoreType.DMA
    packed = jnp.concatenate(
        [normed, key_turned, jnp.zeros((tok_rows, (-ROPE) % 128), jnp.bfloat16)], axis=1
    )
    gathered = call(
        functools.partial(gather_kernel, sp_size),
        jax.ShapeDtypeStruct((sp_size,) + packed.shape, jnp.bfloat16),
        [dma((sp_size,)), dma((sp_size,))],
        0,
        packed,
    ).reshape(sp_size * tok_rows, -1)
    key_set = expand_keys(
        gathered[:, :latent_width],
        large_key_lift,
        large_value_lift,
        small_key_lift,
        small_value_lift,
    )
    key_rot = gathered[:, latent_width : latent_width + ROPE]
    key_positions = jnp.arange(key_rot.shape[0], dtype=jnp.int32)
    causal_mask = positions[:, None] >= key_positions[None, :]
    wide_state = attend_group(
        initial[0], wide_queries, PLAIN_KEY_WIDTH, key_set[0], key_set[1], key_rot, causal_mask
    )
    narrow_state = attend_group(
        initial[1], narrow_queries, SMALL_HEAD_WIDTH, key_set[2], key_set[3], key_rot, causal_mask
    )

    def heads_out(state):
        return (state[2] / state[1][..., None]).astype(jnp.bfloat16).reshape(tok_rows, -1)

    partial_value = jnp.dot(heads_out(wide_state), out_wide, preferred_element_type=jnp.float32)
    partial_value = partial_value + jnp.dot(
        heads_out(narrow_state), out_narrow, preferred_element_type=jnp.float32
    )
    group_count = router_group.shape[1]
    expert_count = router_expert.shape[1]
    model_width = residual.shape[1]
    column_count = model_width // tp_size
    router_width = group_count + expert_count
    router_rows = -(-router_width // 16) * 16
    router = jnp.concatenate([router_group, router_expert], axis=1)
    router = jnp.pad(router, ((0, 0), (0, router_rows - router_width))).T
    mixed, stats = call(
        functools.partial(mix_kernel, tp_size),
        [
            jax.ShapeDtypeStruct((tok_rows, column_count), jnp.float32),
            jax.ShapeDtypeStruct((router_rows + 8, tok_rows), jnp.float32),
        ],
        [
            pltpu.VMEM((tp_size, tok_rows, column_count), jnp.bfloat16),
            pltpu.VMEM((router_rows + 8, tok_rows), jnp.float32),
            pltpu.VMEM((tp_size, router_rows + 8, tok_rows), jnp.float32),
            dma((2, tp_size)),
            dma((2, tp_size)),
        ],
        1,
        partial_value.astype(jnp.bfloat16),
        residual,
        mix_gain[None, :],
        router,
    )
    inverse = lax.rsqrt(stats[router_rows] / model_width + epsilon)
    own_gain = lax.dynamic_slice_in_dim(
        mix_gain, lax.axis_index("tp") * column_count, column_count, 0
    )
    normal_rows = (mixed * inverse[:, None] * own_gain).astype(jnp.bfloat16)
    logits_t = stats[:router_width] * inverse
    group_prob = jax.nn.softmax(logits_t[:group_count], axis=0)
    logits = logits_t[group_count:]
    chosen_group = expert_ids[:, 0] // (expert_count // group_count)
    group_pick = jnp.sum(
        jnp.where(jnp.arange(group_count)[:, None] == chosen_group[None, :], group_prob, 0.0),
        axis=0,
    )
    ids = expert_ids.T
    expert_match = jnp.arange(expert_count)[None, :, None] == ids[:, None, :]
    chosen_logits = jnp.sum(jnp.where(expert_match, logits[None], 0.0), axis=1)
    gates = group_pick * jax.nn.softmax(chosen_logits, axis=0)
    capacity = tp_size * max(1, 4 * tok_rows // (expert_count * tp_size))
    slots = expert_count * capacity
    match = expert_match.astype(jnp.bfloat16)
    named = match[0] + match[1]
    before = (jnp.arange(tok_rows)[:, None] < jnp.arange(tok_rows)[None, :]).astype(jnp.bfloat16)
    earlier = jnp.dot(named, before, preferred_element_type=jnp.float32).astype(jnp.int32)
    slot_index = jnp.sum(jnp.where(expert_match, earlier[None], 0), axis=1)
    target = ids * capacity + slot_index
    pick = (jnp.arange(slots)[None, :, None] == target[:, None, :]).astype(jnp.bfloat16)
    outgoing = jnp.dot(pick[0] + pick[1], normal_rows, preferred_element_type=jnp.float32)
    outgoing = outgoing.astype(jnp.bfloat16).reshape(expert_count, capacity, column_count)
    plane = [dma((sp_size,)), dma((sp_size,)), dma((sp_size, tp_size)), dma((sp_size, tp_size))]
    expert_rows = call(
        functools.partial(dispatch_kernel, sp_size, tp_size),
        jax.ShapeDtypeStruct((sp_size, capacity, model_width), jnp.bfloat16),
        plane,
        2,
        outgoing,
    ).reshape(sp_size * capacity, model_width)
    gate_part = jnp.dot(expert_rows, expert_gate_w[0], preferred_element_type=jnp.float32)
    up_part = jnp.dot(expert_rows, expert_up_w[0], preferred_element_type=jnp.float32)
    hidden = (jax.nn.silu(gate_part) * up_part).astype(jnp.bfloat16)
    down_part = jnp.dot(hidden, expert_down_w[0], preferred_element_type=jnp.float32)
    returned = call(
        functools.partial(combine_kernel, sp_size, tp_size),
        jax.ShapeDtypeStruct((expert_count, capacity, column_count), jnp.bfloat16),
        [
            pltpu.VMEM((sp_size, tp_size, capacity, column_count), jnp.bfloat16),
            pltpu.VMEM((sp_size, capacity, column_count), jnp.bfloat16),
        ]
        + plane,
        3,
        down_part.astype(jnp.bfloat16).reshape(sp_size, capacity, model_width),
    ).reshape(slots, column_count)
    combined = mixed
    for k in range(2):
        picked = lax.dot_general(
            pick[k], returned, (((0,), (0,)), ((), ())), preferred_element_type=jnp.float32
        )
        combined = combined + picked * gates[k][:, None]
    return combined.astype(jnp.bfloat16)


def solution(mesh):
    placed = (
        P("sp", None),
        P("sp", None),
        P("sp", None),
        P(),
        P("sp", "tp"),
        P("sp", "tp"),
        P(None, "tp"),
        P(None, "tp"),
        P(None, "tp"),
        P(None, "tp"),
        P("tp", None),
        P("tp", None),
        P(),
        P(),
        P(),
        P("sp", None),
        P("sp", None, "tp"),
        P("sp", None, "tp"),
        P("sp", "tp", None),
    )
    return jax.shard_map(
        shards, mesh=mesh, in_specs=placed, out_specs=P("sp", "tp"), check_vma=False
    )
```

```python
import functools

import jax
import jax.numpy as jnp
from jax import lax
from jax.experimental import pallas as pl
from jax.experimental.pallas import tpu as pltpu
from jax.sharding import PartitionSpec as P

PLAIN_KEY_WIDTH = 128
LARGE_VALUE_SIZE = 128
SMALL_HEAD_WIDTH = 64
ROPE = 64


rope_base = 10000.0
epsilon = 1e-06
very_low = -1e30


def angle_table(positions, width):
    frequency = rope_base ** (-jnp.arange(0, width, 2, dtype=jnp.float32) / width)
    return positions.astype(jnp.float32)[:, None] * frequency[None, :]


def rotate(values, angles):
    half_width = values.shape[-1] // 2
    cosine = jnp.cos(angles)
    sine_part = jnp.sin(angles)
    front_half = values[..., :half_width]
    back_half = values[..., half_width:]
    return jnp.concatenate(
        [front_half * cosine - back_half * sine_part, front_half * sine_part + back_half * cosine],
        axis=-1,
    )


def rms_scale(values, gain):
    return values * lax.rsqrt(jnp.mean(values * values, axis=-1, keepdims=True) + epsilon) * gain


def roped_queries(query, plain_width, angles):
    row_count = query.shape[0]
    shaped = query.reshape(row_count, -1, plain_width + ROPE)
    turned = rotate(shaped[..., plain_width:].astype(jnp.float32), angles[:, None, :]).astype(
        jnp.bfloat16
    )
    return jnp.concatenate([shaped[..., :plain_width], turned], axis=-1)


def expand_keys(latent_rows, large_key_lift, large_value_lift, small_key_lift, small_value_lift):
    row_count = latent_rows.shape[0]

    def project(weight, head_width):
        product = jnp.dot(latent_rows, weight, preferred_element_type=jnp.float32).astype(
            jnp.bfloat16
        )
        return product.reshape(row_count, weight.shape[1] // head_width, head_width)

    return (
        project(large_key_lift, PLAIN_KEY_WIDTH),
        project(large_value_lift, LARGE_VALUE_SIZE),
        project(small_key_lift, SMALL_HEAD_WIDTH),
        project(small_value_lift, SMALL_HEAD_WIDTH),
    )


def attend_group(state, queries, plain_width, key_rows, values, key_rot, causal_mask):
    row_peak, weight_sum, summed = state
    score_scale = (plain_width + ROPE) ** (-0.5)
    scores = jnp.einsum(
        "qhd,khd->qhk", queries[..., :plain_width], key_rows, preferred_element_type=jnp.float32
    )
    scores = scores + jnp.einsum(
        "qhd,kd->qhk", queries[..., plain_width:], key_rot, preferred_element_type=jnp.float32
    )
    scores = scores * score_scale
    allowed = causal_mask[:, None, :]
    new_peak = jnp.maximum(row_peak, jnp.max(jnp.where(allowed, scores, very_low), axis=-1))
    weights = jnp.where(allowed, jnp.exp(scores - new_peak[..., None]), 0.0)
    weight_sum = jnp.sum(weights, axis=-1)
    summed = jnp.einsum(
        "qhk,khd->qhd", weights.astype(jnp.bfloat16), values, preferred_element_type=jnp.float32
    )
    return (new_peak, weight_sum, summed)


MESH = pl.DeviceIdType.MESH
VMEM_SPEC = pl.BlockSpec(memory_space=pltpu.VMEM)


def flipped(index, bits):
    result, bit = index, 1
    while bit <= bits:
        if bits & bit:
            result = result + bit - 2 * bit * ((index // bit) % 2)
        bit *= 2
    return result


def peer_of(index, step, count):
    if count & (count - 1) == 0:
        return flipped(index, step)
    return lax.rem(index + step, count)


def source_of(index, step, count):
    if count & (count - 1) == 0:
        return flipped(index, step)
    return lax.rem(index + count - step, count)


def to(sp, tp):
    return {"sp": sp, "tp": tp}


def greet(partners):
    barrier = pltpu.get_barrier_semaphore()
    for partner in partners:
        pl.semaphore_signal(barrier, inc=1, device_id=partner, device_id_type=MESH)
    pl.semaphore_wait(barrier, len(partners))


def send(src, dst, send_sem, recv_sem, device):
    copy = pltpu.make_async_remote_copy(
        src_ref=src,
        dst_ref=dst,
        send_sem=send_sem,
        recv_sem=recv_sem,
        device_id=device,
        device_id_type=MESH,
    )
    copy.start()
    return copy


def arrival(dst, send_sem, recv_sem, device):
    pltpu.make_async_remote_copy(
        src_ref=dst,
        dst_ref=dst,
        send_sem=send_sem,
        recv_sem=recv_sem,
        device_id=device,
        device_id_type=MESH,
    ).wait_recv()


def gather_kernel(sp_count, x_ref, out_ref, send_sem, recv_sem):
    me, column = lax.axis_index("sp"), lax.axis_index("tp")
    chips = sp_count // 2
    chip, core = me // 2, me % 2
    partner = 2 * chip + 1 - core
    greet(
        [to(partner, column)]
        + [to(2 * peer_of(chip, d, chips) + core, column) for d in range(1, chips)]
    )
    copies = []
    for d in range(chips - 1, 0, -1):
        there = 2 * peer_of(chip, d, chips) + core
        copies.append(
            send(x_ref, out_ref.at[me], send_sem.at[d], recv_sem.at[me], to(there, column))
        )
    copies.append(
        send(x_ref, out_ref.at[me], send_sem.at[0], recv_sem.at[me], to(partner, column))
    )
    out_ref[me] = x_ref[...]
    for d in range(1, chips):
        origin = 2 * source_of(chip, d, chips) + core
        block = out_ref.at[origin]
        arrival(block, send_sem.at[chips + d], recv_sem.at[origin], to(partner, column))
        copies.append(
            send(block, block, send_sem.at[chips + d], recv_sem.at[origin], to(partner, column))
        )
    for d in range(chips):
        origin = 2 * source_of(chip, d, chips) + 1 - core
        arrival(
            out_ref.at[origin], send_sem.at[0], recv_sem.at[origin], to(partner, column)
        )
    for copy in copies:
        copy.wait_send()


def mix_kernel(
    tp_count,
    part_ref,
    residual_ref,
    gain_ref,
    router_ref,
    mixed_ref,
    stats_ref,
    held,
    own_stats,
    held_stats,
    send_sem,
    recv_sem,
):
    row, me = lax.axis_index("sp"), lax.axis_index("tp")
    width = mixed_ref.shape[1]
    greet([to(row, peer_of(me, d, tp_count)) for d in range(1, tp_count)])

    def columns(index):
        return pl.ds(pl.multiple_of(index * width, width), width)

    copies = []
    for d in range(1, tp_count):
        there = peer_of(me, d, tp_count)
        copies.append(
            send(
                part_ref.at[:, columns(there)],
                held.at[d],
                send_sem.at[0, d],
                recv_sem.at[0, d],
                to(row, there),
            )
        )
    total = residual_ref[:, columns(me)].astype(jnp.float32)
    total = total + part_ref[:, columns(me)].astype(jnp.float32)
    for d in range(1, tp_count):
        arrival(
            held.at[d],
            send_sem.at[0, d],
            recv_sem.at[0, d],
            to(row, peer_of(me, d, tp_count)),
        )
        total = total + held[d].astype(jnp.float32)
    mixed_ref[...] = total
    gained = (total * gain_ref[:, columns(me)]).astype(jnp.bfloat16)
    contract = (((1,), (1,)), ((), ()))
    router_rows = router_ref.shape[0]
    own_stats[:router_rows, :] = lax.dot_general(
        router_ref[:, columns(me)], gained, contract, preferred_element_type=jnp.float32
    )
    own_stats[router_rows:, :] = lax.dot_general(
        jnp.ones((8, width), jnp.float32),
        total * total,
        contract,
        precision=lax.Precision.HIGHEST,
        preferred_element_type=jnp.float32,
    )
    for d in range(1, tp_count):
        copies.append(
            send(
                own_stats,
                held_stats.at[d],
                send_sem.at[1, d],
                recv_sem.at[1, d],
                to(row, peer_of(me, d, tp_count)),
            )
        )
    stats = own_stats[...]
    for d in range(1, tp_count):
        arrival(
            held_stats.at[d],
            send_sem.at[1, d],
            recv_sem.at[1, d],
            to(row, peer_of(me, d, tp_count)),
        )
        stats = stats + held_stats[d]
    stats_ref[...] = stats
    for copy in copies:
        copy.wait_send()


def everyone(row, column, sp_count, tp_count):
    return [to(peer_of(row, d, sp_count), column) for d in range(1, sp_count)] + [
        to(row, peer_of(column, e, tp_count)) for e in range(1, tp_count)
    ]


def expert_kernel(
    sp_count,
    tp_count,
    x_ref,
    gate_hbm,
    up_hbm,
    down_hbm,
    out_ref,
    rows,
    part,
    held,
    summed,
    hidden,
    gate_w,
    up_w,
    down_w,
    load_sem,
    line_send,
    line_recv,
    plane_send,
    plane_recv,
    back_send,
    back_recv,
    sum_send,
    sum_recv,
):
    row, column = lax.axis_index("sp"), lax.axis_index("tp")
    capacity, width = x_ref.shape[1:]
    model_width = part.shape[2]
    loads = [
        pltpu.make_async_copy(gate_hbm, gate_w, load_sem.at[0]),
        pltpu.make_async_copy(up_hbm, up_w, load_sem.at[1]),
        pltpu.make_async_copy(down_hbm, down_w, load_sem.at[2]),
    ]
    for load in loads:
        load.start()
    greet(everyone(row, column, sp_count, tp_count))

    def columns(index):
        return pl.ds(pl.multiple_of(index * width, width), width)

    copies = []
    for d in range(1, sp_count):
        there = peer_of(row, d, sp_count)
        copies.append(
            send(
                x_ref.at[there],
                rows.at[d, :, columns(column)],
                line_send.at[d],
                line_recv.at[d],
                to(there, column),
            )
        )

    def spread(d):
        block = rows.at[d, :, columns(column)]
        if d > 0:
            arrival(
                block,
                line_send.at[d],
                line_recv.at[d],
                to(source_of(row, d, sp_count), column),
            )
        for e in range(1, tp_count):
            copies.append(
                send(
                    block if d > 0 else x_ref.at[row],
                    block,
                    plane_send.at[d, e],
                    plane_recv.at[d, e],
                    to(row, peer_of(column, e, tp_count)),
                )
            )
        if d == 0:
            rows[0, :, columns(column)] = x_ref[row]

    def run(first, count):
        for d in range(first, first + count):
            for e in range(1, tp_count):
                origin = source_of(column, e, tp_count)
                arrival(
                    rows.at[d, :, columns(origin)],
                    plane_send.at[d, e],
                    plane_recv.at[d, e],
                    to(row, origin),
                )
        tall = count * capacity
        if first == 0:
            loads[0].wait()
            loads[1].wait()
        unit_tile = min(256, hidden.shape[1])

        def units(n, carry):
            here = pl.ds(pl.multiple_of(n * unit_tile, unit_tile), unit_tile)
            tokens = rows[first : first + count].reshape(tall, model_width)
            gate = jnp.dot(tokens, gate_w[:, here], preferred_element_type=jnp.float32)
            up = jnp.dot(tokens, up_w[:, here], preferred_element_type=jnp.float32)
            hidden[:, here] = (gate / (1.0 + jnp.exp(-gate)) * up).astype(jnp.bfloat16)
            return carry

        lax.fori_loop(0, hidden.shape[1] // unit_tile, units, 0)
        if first == 0:
            loads[2].wait()
        tile = min(256, model_width)

        def outputs(n, carry):
            here = pl.ds(pl.multiple_of(n * tile, tile), tile)
            product = jnp.dot(hidden[...], down_w[:, here], preferred_element_type=jnp.float32)
            part[first : first + count, :, here] = product.astype(jnp.bfloat16).reshape(
                count, capacity, tile
            )
            return carry

        lax.fori_loop(0, model_width // tile, outputs, 0)
        for d in range(first, first + count):
            for e in range(1, tp_count):
                there = peer_of(column, e, tp_count)
                copies.append(
                    send(
                        part.at[d, :, columns(there)],
                        held.at[d, e],
                        back_send.at[d, e],
                        back_recv.at[d, e],
                        to(row, there),
                    )
                )

    def finish(d):
        total = part[d, :, columns(column)].astype(jnp.float32)
        for e in range(1, tp_count):
            arrival(
                held.at[d, e],
                back_send.at[d, e],
                back_recv.at[d, e],
                to(row, source_of(column, e, tp_count)),
            )
            total = total + held[d, e].astype(jnp.float32)
        if d == 0:
            out_ref[row] = total.astype(jnp.bfloat16)
        else:
            owner = source_of(row, d, sp_count)
            summed[d] = total.astype(jnp.bfloat16)
            copies.append(
                send(
                    summed.at[d],
                    out_ref.at[row],
                    sum_send.at[d],
                    sum_recv.at[d],
                    to(owner, column),
                )
            )

    count = 2
    for d in range(count):
        spread(d)
    for first in range(0, sp_count, count):
        if first + count < sp_count:
            for d in range(first + count, first + 2 * count):
                spread(d)
        run(first, count)
        if first > 0:
            for d in range(first - count, first):
                finish(d)
    for d in range(sp_count - count, sp_count):
        finish(d)
    for d in range(1, sp_count):
        expert = peer_of(row, d, sp_count)
        arrival(out_ref.at[expert], sum_send.at[d], sum_recv.at[d], to(expert, column))
    for copy in copies:
        copy.wait_send()


def call(body, out_shape, scratch, collective_id, *operands, streamed=0):
    many = isinstance(out_shape, (list, tuple))
    return pl.pallas_call(
        body,
        out_shape=out_shape,
        in_specs=[VMEM_SPEC] * (len(operands) - streamed)
        + [pl.BlockSpec(memory_space=pl.ANY)] * streamed,
        out_specs=[VMEM_SPEC] * len(out_shape) if many else VMEM_SPEC,
        scratch_shapes=scratch,
        compiler_params=pltpu.CompilerParams(
            collective_id=collective_id, has_side_effects=True
        ),
    )(*operands)


def shards(
    residual,
    latent,
    rot_key,
    latent_norm_scale,
    query_wide,
    query_narrow,
    large_key_lift,
    large_value_lift,
    small_key_lift,
    small_value_lift,
    out_wide,
    out_narrow,
    mix_gain,
    router_group,
    router_expert,
    expert_ids,
    expert_gate_w,
    expert_up_w,
    expert_down_w,
):
    tok_rows = latent.shape[0]
    positions = lax.axis_index("sp") * tok_rows + jnp.arange(tok_rows, dtype=jnp.int32)
    angles = angle_table(positions, ROPE)
    normed = rms_scale(latent.astype(jnp.float32), latent_norm_scale).astype(jnp.bfloat16)
    key_turned = rotate(rot_key.astype(jnp.float32), angles).astype(jnp.bfloat16)
    wide_queries = roped_queries(query_wide, PLAIN_KEY_WIDTH, angles)
    narrow_queries = roped_queries(query_narrow, SMALL_HEAD_WIDTH, angles)

    def empty_state(head_count, head_width):
        return (
            jnp.full((tok_rows, head_count), very_low, jnp.float32),
            jnp.zeros((tok_rows, head_count), jnp.float32),
            jnp.zeros((tok_rows, head_count, head_width), jnp.float32),
        )

    initial = (
        empty_state(wide_queries.shape[1], LARGE_VALUE_SIZE),
        empty_state(narrow_queries.shape[1], SMALL_HEAD_WIDTH),
    )
    sp_size, tp_size = lax.axis_size("sp"), lax.axis_size("tp")
    latent_width = latent.shape[1]
    dma = pltpu.SemaphoreType.DMA
    packed = jnp.concatenate(
        [normed, key_turned, jnp.zeros((tok_rows, (-ROPE) % 128), jnp.bfloat16)], axis=1
    )
    gathered = call(
        functools.partial(gather_kernel, sp_size),
        jax.ShapeDtypeStruct((sp_size,) + packed.shape, jnp.bfloat16),
        [dma((sp_size,)), dma((sp_size,))],
        0,
        packed,
    ).reshape(sp_size * tok_rows, -1)
    key_set = expand_keys(
        gathered[:, :latent_width],
        large_key_lift,
        large_value_lift,
        small_key_lift,
        small_value_lift,
    )
    key_rot = gathered[:, latent_width : latent_width + ROPE]
    key_positions = jnp.arange(key_rot.shape[0], dtype=jnp.int32)
    causal_mask = positions[:, None] >= key_positions[None, :]
    wide_state = attend_group(
        initial[0], wide_queries, PLAIN_KEY_WIDTH, key_set[0], key_set[1], key_rot, causal_mask
    )
    narrow_state = attend_group(
        initial[1], narrow_queries, SMALL_HEAD_WIDTH, key_set[2], key_set[3], key_rot, causal_mask
    )

    def heads_out(state):
        return (state[2] / state[1][..., None]).astype(jnp.bfloat16).reshape(tok_rows, -1)

    partial_value = jnp.dot(heads_out(wide_state), out_wide, preferred_element_type=jnp.float32)
    partial_value = partial_value + jnp.dot(
        heads_out(narrow_state), out_narrow, preferred_element_type=jnp.float32
    )
    group_count = router_group.shape[1]
    expert_count = router_expert.shape[1]
    model_width = residual.shape[1]
    column_count = model_width // tp_size
    router_width = group_count + expert_count
    router_rows = -(-router_width // 16) * 16
    router = jnp.concatenate([router_group, router_expert], axis=1)
    router = jnp.pad(router, ((0, 0), (0, router_rows - router_width))).T
    mixed, stats = call(
        functools.partial(mix_kernel, tp_size),
        [
            jax.ShapeDtypeStruct((tok_rows, column_count), jnp.float32),
            jax.ShapeDtypeStruct((router_rows + 8, tok_rows), jnp.float32),
        ],
        [
            pltpu.VMEM((tp_size, tok_rows, column_count), jnp.bfloat16),
            pltpu.VMEM((router_rows + 8, tok_rows), jnp.float32),
            pltpu.VMEM((tp_size, router_rows + 8, tok_rows), jnp.float32),
            dma((2, tp_size)),
            dma((2, tp_size)),
        ],
        1,
        partial_value.astype(jnp.bfloat16),
        residual,
        mix_gain[None, :],
        router,
    )
    inverse = lax.rsqrt(stats[router_rows] / model_width + epsilon)
    own_gain = lax.dynamic_slice_in_dim(
        mix_gain, lax.axis_index("tp") * column_count, column_count, 0
    )
    normal_rows = (mixed * inverse[:, None] * own_gain).astype(jnp.bfloat16)
    logits_t = stats[:router_width] * inverse
    group_prob = jax.nn.softmax(logits_t[:group_count], axis=0)
    logits = logits_t[group_count:]
    chosen_group = expert_ids[:, 0] // (expert_count // group_count)
    group_pick = jnp.sum(
        jnp.where(jnp.arange(group_count)[:, None] == chosen_group[None, :], group_prob, 0.0),
        axis=0,
    )
    ids = expert_ids.T
    expert_match = jnp.arange(expert_count)[None, :, None] == ids[:, None, :]
    chosen_logits = jnp.sum(jnp.where(expert_match, logits[None], 0.0), axis=1)
    gates = group_pick * jax.nn.softmax(chosen_logits, axis=0)
    capacity = tp_size * max(1, 4 * tok_rows // (expert_count * tp_size))
    slots = expert_count * capacity
    match = expert_match.astype(jnp.bfloat16)
    named = match[0] + match[1]
    before = (jnp.arange(tok_rows)[:, None] < jnp.arange(tok_rows)[None, :]).astype(jnp.bfloat16)
    earlier = jnp.dot(named, before, preferred_element_type=jnp.float32).astype(jnp.int32)
    slot_index = jnp.sum(jnp.where(expert_match, earlier[None], 0), axis=1)
    target = ids * capacity + slot_index
    pick = (jnp.arange(slots)[None, :, None] == target[:, None, :]).astype(jnp.bfloat16)
    outgoing = jnp.dot(pick[0] + pick[1], normal_rows, preferred_element_type=jnp.float32)
    outgoing = outgoing.astype(jnp.bfloat16).reshape(expert_count, capacity, column_count)
    line, plane = dma((sp_size,)), dma((sp_size, tp_size))
    units = expert_down_w.shape[1]
    bf16 = jnp.bfloat16
    returned = call(
        functools.partial(expert_kernel, sp_size, tp_size),
        jax.ShapeDtypeStruct((expert_count, capacity, column_count), bf16),
        [
            pltpu.VMEM((sp_size, capacity, model_width), bf16),
            pltpu.VMEM((sp_size, capacity, model_width), bf16),
            pltpu.VMEM((sp_size, tp_size, capacity, column_count), bf16),
            pltpu.VMEM((sp_size, capacity, column_count), bf16),
            pltpu.VMEM((2 * capacity, units), bf16),
            pltpu.VMEM((model_width, units), bf16),
            pltpu.VMEM((model_width, units), bf16),
            pltpu.VMEM((units, model_width), bf16),
            dma((3,)),
            line,
            line,
            plane,
            plane,
            plane,
            plane,
            line,
            line,
        ],
        2,
        outgoing,
        expert_gate_w[0],
        expert_up_w[0],
        expert_down_w[0],
        streamed=3,
    ).reshape(slots, column_count)
    combined = mixed
    for k in range(2):
        picked = lax.dot_general(
            pick[k], returned, (((0,), (0,)), ((), ())), preferred_element_type=jnp.float32
        )
        combined = combined + picked * gates[k][:, None]
    return combined.astype(jnp.bfloat16)


def solution(mesh):
    placed = (
        P("sp", None),
        P("sp", None),
        P("sp", None),
        P(),
        P("sp", "tp"),
        P("sp", "tp"),
        P(None, "tp"),
        P(None, "tp"),
        P(None, "tp"),
        P(None, "tp"),
        P("tp", None),
        P("tp", None),
        P(),
        P(),
        P(),
        P("sp", None),
        P("sp", None, "tp"),
        P("sp", None, "tp"),
        P("sp", "tp", None),
    )
    return jax.shard_map(
        shards, mesh=mesh, in_specs=placed, out_specs=P("sp", "tp"), check_vma=False
    )
```

```python
import functools

import jax
import jax.numpy as jnp
from jax import lax
from jax.experimental import pallas as pl
from jax.experimental.pallas import tpu as pltpu
from jax.sharding import PartitionSpec as P

PLAIN_KEY_WIDTH = 128
LARGE_VALUE_SIZE = 128
SMALL_HEAD_WIDTH = 64
ROPE = 64


rope_base = 10000.0
epsilon = 1e-06
very_low = -1e30


def angle_table(positions, width):
    frequency = rope_base ** (-jnp.arange(0, width, 2, dtype=jnp.float32) / width)
    return positions.astype(jnp.float32)[:, None] * frequency[None, :]


def rotate(values, angles):
    half_width = values.shape[-1] // 2
    cosine = jnp.cos(angles)
    sine_part = jnp.sin(angles)
    front_half = values[..., :half_width]
    back_half = values[..., half_width:]
    return jnp.concatenate(
        [front_half * cosine - back_half * sine_part, front_half * sine_part + back_half * cosine],
        axis=-1,
    )


def rms_scale(values, gain):
    return values * lax.rsqrt(jnp.mean(values * values, axis=-1, keepdims=True) + epsilon) * gain


def roped_queries(query, plain_width, angles):
    row_count = query.shape[0]
    shaped = query.reshape(row_count, -1, plain_width + ROPE)
    turned = rotate(shaped[..., plain_width:].astype(jnp.float32), angles[:, None, :]).astype(
        jnp.bfloat16
    )
    return jnp.concatenate([shaped[..., :plain_width], turned], axis=-1)


def expand_keys(latent_rows, large_key_lift, large_value_lift, small_key_lift, small_value_lift):
    row_count = latent_rows.shape[0]

    def project(weight, head_width):
        product = jnp.dot(latent_rows, weight, preferred_element_type=jnp.float32).astype(
            jnp.bfloat16
        )
        return product.reshape(row_count, weight.shape[1] // head_width, head_width)

    return (
        project(large_key_lift, PLAIN_KEY_WIDTH),
        project(large_value_lift, LARGE_VALUE_SIZE),
        project(small_key_lift, SMALL_HEAD_WIDTH),
        project(small_value_lift, SMALL_HEAD_WIDTH),
    )


def attend_group(state, queries, plain_width, key_rows, values, key_rot, causal_mask):
    row_peak, weight_sum, summed = state
    score_scale = (plain_width + ROPE) ** (-0.5)
    scores = jnp.einsum(
        "qhd,khd->qhk", queries[..., :plain_width], key_rows, preferred_element_type=jnp.float32
    )
    scores = scores + jnp.einsum(
        "qhd,kd->qhk", queries[..., plain_width:], key_rot, preferred_element_type=jnp.float32
    )
    scores = scores * score_scale
    allowed = causal_mask[:, None, :]
    new_peak = jnp.maximum(row_peak, jnp.max(jnp.where(allowed, scores, very_low), axis=-1))
    weights = jnp.where(allowed, jnp.exp(scores - new_peak[..., None]), 0.0)
    weight_sum = jnp.sum(weights, axis=-1)
    summed = jnp.einsum(
        "qhk,khd->qhd", weights.astype(jnp.bfloat16), values, preferred_element_type=jnp.float32
    )
    return (new_peak, weight_sum, summed)


MESH = pl.DeviceIdType.MESH
VMEM_SPEC = pl.BlockSpec(memory_space=pltpu.VMEM)


def flipped(index, bits):
    result, bit = index, 1
    while bit <= bits:
        if bits & bit:
            result = result + bit - 2 * bit * ((index // bit) % 2)
        bit *= 2
    return result


def peer_of(index, step, count):
    if count & (count - 1) == 0:
        return flipped(index, step)
    return lax.rem(index + step, count)


def source_of(index, step, count):
    if count & (count - 1) == 0:
        return flipped(index, step)
    return lax.rem(index + count - step, count)


def to(sp, tp):
    return {"sp": sp, "tp": tp}


def greet(partners):
    barrier = pltpu.get_barrier_semaphore()
    for partner in partners:
        pl.semaphore_signal(barrier, inc=1, device_id=partner, device_id_type=MESH)
    pl.semaphore_wait(barrier, len(partners))


def send(src, dst, send_sem, recv_sem, device):
    copy = pltpu.make_async_remote_copy(
        src_ref=src,
        dst_ref=dst,
        send_sem=send_sem,
        recv_sem=recv_sem,
        device_id=device,
        device_id_type=MESH,
    )
    copy.start()
    return copy


def arrival(dst, send_sem, recv_sem, device):
    pltpu.make_async_remote_copy(
        src_ref=dst,
        dst_ref=dst,
        send_sem=send_sem,
        recv_sem=recv_sem,
        device_id=device,
        device_id_type=MESH,
    ).wait_recv()


def gather_kernel(sp_count, x_ref, out_ref, send_sem, recv_sem):
    me, column = lax.axis_index("sp"), lax.axis_index("tp")
    chips = sp_count // 2
    chip, core = me // 2, me % 2
    partner = 2 * chip + 1 - core
    greet(
        [to(partner, column)]
        + [to(2 * peer_of(chip, d, chips) + core, column) for d in range(1, chips)]
    )
    copies = []
    for d in range(chips - 1, 0, -1):
        there = 2 * peer_of(chip, d, chips) + core
        copies.append(
            send(x_ref, out_ref.at[me], send_sem.at[d], recv_sem.at[me], to(there, column))
        )
    copies.append(
        send(x_ref, out_ref.at[me], send_sem.at[0], recv_sem.at[me], to(partner, column))
    )
    out_ref[me] = x_ref[...]
    for d in range(1, chips):
        origin = 2 * source_of(chip, d, chips) + core
        block = out_ref.at[origin]
        arrival(block, send_sem.at[chips + d], recv_sem.at[origin], to(partner, column))
        copies.append(
            send(block, block, send_sem.at[chips + d], recv_sem.at[origin], to(partner, column))
        )
    for d in range(chips):
        origin = 2 * source_of(chip, d, chips) + 1 - core
        arrival(
            out_ref.at[origin], send_sem.at[0], recv_sem.at[origin], to(partner, column)
        )
    for copy in copies:
        copy.wait_send()


def mix_kernel(
    tp_count,
    part_ref,
    residual_ref,
    gain_ref,
    router_ref,
    mixed_ref,
    gained_ref,
    stats_ref,
    held,
    own_stats,
    held_stats,
    send_sem,
    recv_sem,
):
    row, me = lax.axis_index("sp"), lax.axis_index("tp")
    width = mixed_ref.shape[1]
    greet([to(row, peer_of(me, d, tp_count)) for d in range(1, tp_count)])

    def columns(index):
        return pl.ds(pl.multiple_of(index * width, width), width)

    copies = []
    for d in range(1, tp_count):
        there = peer_of(me, d, tp_count)
        copies.append(
            send(
                part_ref.at[:, columns(there)],
                held.at[d],
                send_sem.at[0, d],
                recv_sem.at[0, d],
                to(row, there),
            )
        )
    total = residual_ref[:, columns(me)].astype(jnp.float32)
    total = total + part_ref[:, columns(me)].astype(jnp.float32)
    for d in range(1, tp_count):
        arrival(
            held.at[d],
            send_sem.at[0, d],
            recv_sem.at[0, d],
            to(row, peer_of(me, d, tp_count)),
        )
        total = total + held[d].astype(jnp.float32)
    mixed_ref[...] = total
    gained_ref[...] = total * gain_ref[:, columns(me)]
    gained = gained_ref[...].astype(jnp.bfloat16)
    contract = (((1,), (1,)), ((), ()))
    router_rows = router_ref.shape[0]
    own_stats[:router_rows, :] = lax.dot_general(
        router_ref[:, columns(me)], gained, contract, preferred_element_type=jnp.float32
    )
    own_stats[router_rows:, :] = lax.dot_general(
        jnp.ones((8, width), jnp.float32),
        total * total,
        contract,
        precision=lax.Precision.HIGHEST,
        preferred_element_type=jnp.float32,
    )
    for d in range(1, tp_count):
        copies.append(
            send(
                own_stats,
                held_stats.at[d],
                send_sem.at[1, d],
                recv_sem.at[1, d],
                to(row, peer_of(me, d, tp_count)),
            )
        )
    stats = own_stats[...]
    for d in range(1, tp_count):
        arrival(
            held_stats.at[d],
            send_sem.at[1, d],
            recv_sem.at[1, d],
            to(row, peer_of(me, d, tp_count)),
        )
        stats = stats + held_stats[d]
    stats_ref[...] = stats
    for copy in copies:
        copy.wait_send()


def everyone(row, column, sp_count, tp_count):
    return [to(peer_of(row, d, sp_count), column) for d in range(1, sp_count)] + [
        to(row, peer_of(column, e, tp_count)) for e in range(1, tp_count)
    ]


def expert_kernel(
    sp_count,
    tp_count,
    x_ref,
    gate_hbm,
    up_hbm,
    down_hbm,
    out_ref,
    rows,
    part,
    held,
    summed,
    hidden,
    gate_w,
    up_w,
    down_w,
    load_sem,
    line_send,
    line_recv,
    plane_send,
    plane_recv,
    back_send,
    back_recv,
    sum_send,
    sum_recv,
):
    row, column = lax.axis_index("sp"), lax.axis_index("tp")
    capacity, width = x_ref.shape[1:]
    model_width = part.shape[2]
    loads = [
        pltpu.make_async_copy(gate_hbm, gate_w, load_sem.at[0]),
        pltpu.make_async_copy(up_hbm, up_w, load_sem.at[1]),
        pltpu.make_async_copy(down_hbm, down_w, load_sem.at[2]),
    ]
    for load in loads:
        load.start()
    greet(everyone(row, column, sp_count, tp_count))

    def columns(index):
        return pl.ds(pl.multiple_of(index * width, width), width)

    copies = []
    for d in range(1, sp_count):
        there = peer_of(row, d, sp_count)
        copies.append(
            send(
                x_ref.at[there],
                rows.at[d, :, columns(column)],
                line_send.at[d],
                line_recv.at[d],
                to(there, column),
            )
        )

    def spread(d):
        block = rows.at[d, :, columns(column)]
        if d > 0:
            arrival(
                block,
                line_send.at[d],
                line_recv.at[d],
                to(source_of(row, d, sp_count), column),
            )
        for e in range(1, tp_count):
            copies.append(
                send(
                    block if d > 0 else x_ref.at[row],
                    block,
                    plane_send.at[d, e],
                    plane_recv.at[d, e],
                    to(row, peer_of(column, e, tp_count)),
                )
            )
        if d == 0:
            rows[0, :, columns(column)] = x_ref[row]

    def run(first, count):
        for d in range(first, first + count):
            for e in range(1, tp_count):
                origin = source_of(column, e, tp_count)
                arrival(
                    rows.at[d, :, columns(origin)],
                    plane_send.at[d, e],
                    plane_recv.at[d, e],
                    to(row, origin),
                )
        tall = count * capacity
        if first == 0:
            loads[0].wait()
            loads[1].wait()
        unit_tile = min(256, hidden.shape[1])

        def units(n, carry):
            here = pl.ds(pl.multiple_of(n * unit_tile, unit_tile), unit_tile)
            tokens = rows[first : first + count].reshape(tall, model_width)
            gate = jnp.dot(tokens, gate_w[:, here], preferred_element_type=jnp.float32)
            up = jnp.dot(tokens, up_w[:, here], preferred_element_type=jnp.float32)
            hidden[:, here] = (gate / (1.0 + jnp.exp(-gate)) * up).astype(jnp.bfloat16)
            return carry

        lax.fori_loop(0, hidden.shape[1] // unit_tile, units, 0)
        if first == 0:
            loads[2].wait()
        tile = min(256, model_width)

        def outputs(n, carry):
            here = pl.ds(pl.multiple_of(n * tile, tile), tile)
            product = jnp.dot(hidden[...], down_w[:, here], preferred_element_type=jnp.float32)
            part[first : first + count, :, here] = product.astype(jnp.bfloat16).reshape(
                count, capacity, tile
            )
            return carry

        lax.fori_loop(0, model_width // tile, outputs, 0)
        for d in range(first, first + count):
            for e in range(1, tp_count):
                there = peer_of(column, e, tp_count)
                copies.append(
                    send(
                        part.at[d, :, columns(there)],
                        held.at[d, e],
                        back_send.at[d, e],
                        back_recv.at[d, e],
                        to(row, there),
                    )
                )

    def finish(d):
        total = part[d, :, columns(column)].astype(jnp.float32)
        for e in range(1, tp_count):
            arrival(
                held.at[d, e],
                back_send.at[d, e],
                back_recv.at[d, e],
                to(row, source_of(column, e, tp_count)),
            )
            total = total + held[d, e].astype(jnp.float32)
        if d == 0:
            out_ref[row] = total.astype(jnp.bfloat16)
        else:
            owner = source_of(row, d, sp_count)
            summed[d] = total.astype(jnp.bfloat16)
            copies.append(
                send(
                    summed.at[d],
                    out_ref.at[row],
                    sum_send.at[d],
                    sum_recv.at[d],
                    to(owner, column),
                )
            )

    count = 2
    for d in range(count):
        spread(d)
    for first in range(0, sp_count, count):
        if first + count < sp_count:
            for d in range(first + count, first + 2 * count):
                spread(d)
        run(first, count)
        if first > 0:
            for d in range(first - count, first):
                finish(d)
    for d in range(sp_count - count, sp_count):
        finish(d)
    for d in range(1, sp_count):
        expert = peer_of(row, d, sp_count)
        arrival(out_ref.at[expert], sum_send.at[d], sum_recv.at[d], to(expert, column))
    for copy in copies:
        copy.wait_send()


def call(body, out_shape, scratch, collective_id, *operands, streamed=0):
    many = isinstance(out_shape, (list, tuple))
    return pl.pallas_call(
        body,
        out_shape=out_shape,
        in_specs=[VMEM_SPEC] * (len(operands) - streamed)
        + [pl.BlockSpec(memory_space=pl.ANY)] * streamed,
        out_specs=[VMEM_SPEC] * len(out_shape) if many else VMEM_SPEC,
        scratch_shapes=scratch,
        compiler_params=pltpu.CompilerParams(
            collective_id=collective_id, has_side_effects=True
        ),
    )(*operands)


def shards(
    residual,
    latent,
    rot_key,
    latent_norm_scale,
    query_wide,
    query_narrow,
    large_key_lift,
    large_value_lift,
    small_key_lift,
    small_value_lift,
    out_wide,
    out_narrow,
    mix_gain,
    router_group,
    router_expert,
    expert_ids,
    expert_gate_w,
    expert_up_w,
    expert_down_w,
):
    tok_rows = latent.shape[0]
    positions = lax.axis_index("sp") * tok_rows + jnp.arange(tok_rows, dtype=jnp.int32)
    angles = angle_table(positions, ROPE)
    normed = rms_scale(latent.astype(jnp.float32), latent_norm_scale).astype(jnp.bfloat16)
    key_turned = rotate(rot_key.astype(jnp.float32), angles).astype(jnp.bfloat16)
    wide_queries = roped_queries(query_wide, PLAIN_KEY_WIDTH, angles)
    narrow_queries = roped_queries(query_narrow, SMALL_HEAD_WIDTH, angles)

    def empty_state(head_count, head_width):
        return (
            jnp.full((tok_rows, head_count), very_low, jnp.float32),
            jnp.zeros((tok_rows, head_count), jnp.float32),
            jnp.zeros((tok_rows, head_count, head_width), jnp.float32),
        )

    initial = (
        empty_state(wide_queries.shape[1], LARGE_VALUE_SIZE),
        empty_state(narrow_queries.shape[1], SMALL_HEAD_WIDTH),
    )
    sp_size, tp_size = lax.axis_size("sp"), lax.axis_size("tp")
    latent_width = latent.shape[1]
    dma = pltpu.SemaphoreType.DMA
    packed = jnp.concatenate(
        [normed, key_turned, jnp.zeros((tok_rows, (-ROPE) % 128), jnp.bfloat16)], axis=1
    )
    gathered = call(
        functools.partial(gather_kernel, sp_size),
        jax.ShapeDtypeStruct((sp_size,) + packed.shape, jnp.bfloat16),
        [dma((sp_size,)), dma((sp_size,))],
        0,
        packed,
    ).reshape(sp_size * tok_rows, -1)
    key_set = expand_keys(
        gathered[:, :latent_width],
        large_key_lift,
        large_value_lift,
        small_key_lift,
        small_value_lift,
    )
    key_rot = gathered[:, latent_width : latent_width + ROPE]
    key_positions = jnp.arange(key_rot.shape[0], dtype=jnp.int32)
    causal_mask = positions[:, None] >= key_positions[None, :]
    wide_state = attend_group(
        initial[0], wide_queries, PLAIN_KEY_WIDTH, key_set[0], key_set[1], key_rot, causal_mask
    )
    narrow_state = attend_group(
        initial[1], narrow_queries, SMALL_HEAD_WIDTH, key_set[2], key_set[3], key_rot, causal_mask
    )

    def heads_out(state):
        return (state[2] / state[1][..., None]).astype(jnp.bfloat16).reshape(tok_rows, -1)

    partial_value = jnp.dot(heads_out(wide_state), out_wide, preferred_element_type=jnp.float32)
    partial_value = partial_value + jnp.dot(
        heads_out(narrow_state), out_narrow, preferred_element_type=jnp.float32
    )
    group_count = router_group.shape[1]
    expert_count = router_expert.shape[1]
    model_width = residual.shape[1]
    column_count = model_width // tp_size
    router_width = group_count + expert_count
    router_rows = -(-router_width // 16) * 16
    router = jnp.concatenate([router_group, router_expert], axis=1)
    router = jnp.pad(router, ((0, 0), (0, router_rows - router_width))).T
    mixed, gained, stats = call(
        functools.partial(mix_kernel, tp_size),
        [
            jax.ShapeDtypeStruct((tok_rows, column_count), jnp.float32),
            jax.ShapeDtypeStruct((tok_rows, column_count), jnp.float32),
            jax.ShapeDtypeStruct((router_rows + 8, tok_rows), jnp.float32),
        ],
        [
            pltpu.VMEM((tp_size, tok_rows, column_count), jnp.bfloat16),
            pltpu.VMEM((router_rows + 8, tok_rows), jnp.float32),
            pltpu.VMEM((tp_size, router_rows + 8, tok_rows), jnp.float32),
            dma((2, tp_size)),
            dma((2, tp_size)),
        ],
        1,
        partial_value.astype(jnp.bfloat16),
        residual,
        mix_gain[None, :],
        router,
    )
    inverse = lax.rsqrt(stats[router_rows] / model_width + epsilon)
    normal_rows = (gained * inverse[:, None]).astype(jnp.bfloat16)
    logits_t = stats[:router_width] * inverse
    group_prob = jax.nn.softmax(logits_t[:group_count], axis=0)
    logits = logits_t[group_count:]
    chosen_group = expert_ids[:, 0] // (expert_count // group_count)
    group_pick = jnp.sum(
        jnp.where(jnp.arange(group_count)[:, None] == chosen_group[None, :], group_prob, 0.0),
        axis=0,
    )
    ids = expert_ids.T
    expert_match = jnp.arange(expert_count)[None, :, None] == ids[:, None, :]
    chosen_logits = jnp.sum(jnp.where(expert_match, logits[None], 0.0), axis=1)
    gates = group_pick * jax.nn.softmax(chosen_logits, axis=0)
    capacity = tp_size * max(1, 4 * tok_rows // (expert_count * tp_size))
    slots = expert_count * capacity
    match = expert_match.astype(jnp.bfloat16)
    named = match[0] + match[1]
    before = (jnp.arange(tok_rows)[:, None] < jnp.arange(tok_rows)[None, :]).astype(jnp.bfloat16)
    earlier = jnp.dot(named, before, preferred_element_type=jnp.float32).astype(jnp.int32)
    slot_index = jnp.sum(jnp.where(expert_match, earlier[None], 0), axis=1)
    target = ids * capacity + slot_index
    pick = (jnp.arange(slots)[None, :, None] == target[:, None, :]).astype(jnp.bfloat16)
    outgoing = jnp.dot(pick[0] + pick[1], normal_rows, preferred_element_type=jnp.float32)
    outgoing = outgoing.astype(jnp.bfloat16).reshape(expert_count, capacity, column_count)
    line, plane = dma((sp_size,)), dma((sp_size, tp_size))
    units = expert_down_w.shape[1]
    bf16 = jnp.bfloat16
    returned = call(
        functools.partial(expert_kernel, sp_size, tp_size),
        jax.ShapeDtypeStruct((expert_count, capacity, column_count), bf16),
        [
            pltpu.VMEM((sp_size, capacity, model_width), bf16),
            pltpu.VMEM((sp_size, capacity, model_width), bf16),
            pltpu.VMEM((sp_size, tp_size, capacity, column_count), bf16),
            pltpu.VMEM((sp_size, capacity, column_count), bf16),
            pltpu.VMEM((2 * capacity, units), bf16),
            pltpu.VMEM((model_width, units), bf16),
            pltpu.VMEM((model_width, units), bf16),
            pltpu.VMEM((units, model_width), bf16),
            dma((3,)),
            line,
            line,
            plane,
            plane,
            plane,
            plane,
            line,
            line,
        ],
        2,
        outgoing,
        expert_gate_w[0],
        expert_up_w[0],
        expert_down_w[0],
        streamed=3,
    ).reshape(slots, column_count)
    back = (target[:, :, None] == jnp.arange(slots)[None, None, :]).astype(bf16)
    picked = jnp.dot(
        back.reshape(2 * tok_rows, slots), returned, preferred_element_type=jnp.float32
    ).reshape(2, tok_rows, column_count)
    combined = mixed + jnp.sum(picked * gates[:, :, None], axis=0)
    return combined.astype(jnp.bfloat16)


def solution(mesh):
    placed = (
        P("sp", None),
        P("sp", None),
        P("sp", None),
        P(),
        P("sp", "tp"),
        P("sp", "tp"),
        P(None, "tp"),
        P(None, "tp"),
        P(None, "tp"),
        P(None, "tp"),
        P("tp", None),
        P("tp", None),
        P(),
        P(),
        P(),
        P("sp", None),
        P("sp", None, "tp"),
        P("sp", None, "tp"),
        P("sp", "tp", None),
    )
    return jax.shard_map(
        shards, mesh=mesh, in_specs=placed, out_specs=P("sp", "tp"), check_vma=False
    )
```
